32 devices in a mesh: fs: 4 (over z), rep: 4 (over y, x), tp: 2 (over core).
Axes of the slice: x: 2, y: 2, z: 4, core: 2. Of those that a mesh axis runs over, the one named last changes fastest.
Arguments:
- inputs: bfloat16 [4096, 2048], P(('fs', 'rep')), may hold values from -6 to 6
- cot_query: bfloat16 [4096, 2048], P(('fs', 'rep'), 'tp'), may hold values from -0.09375 to 0.09375
- cot_key: bfloat16 [4096, 512], P(('fs', 'rep'), 'tp'), may hold values from -0.09375 to 0.09375
- basis_query: bfloat16 [2048, 512], P('fs'), may hold values from -0.125 to 0.125
- basis_key: bfloat16 [2048, 512], P('fs'), may hold values from -0.125 to 0.125
- weight_query: float32 [2048, 2048], P('fs', 'tp'), may hold values from -0.125 to 0.125
- weight_key: float32 [2048, 512], P('fs', 'tp'), may hold values from -0.125 to 0.125
- moments_query: float32 [2, 512, 2048], P(None, 'fs', 'tp'), may hold values from -8 to 8, as said below
- moments_key: float32 [2, 512, 512], P(None, 'fs', 'tp'), may hold values from -8 to 8, as said below
Outputs:
- step_query: float32 [2048, 2048], P('fs', 'tp')
- step_key: float32 [2048, 512], P('fs', 'tp')
- new_weight_query: float32 [2048, 2048], P('fs', 'tp')
- new_weight_key: float32 [2048, 512], P('fs', 'tp')
- copy_query: bfloat16 [2048, 2048], P(None, 'tp')
- copy_key: bfloat16 [2048, 512], P(None, 'tp')
- new_moments_query: float32 [2, 512, 2048], P(None, 'fs', 'tp')
- new_moments_key: float32 [2, 512, 512], P(None, 'fs', 'tp')
The draws below stay inside these ranges and needn't reach their ends.
Inputs may be any that keep to these rules, and one draw needn't show every extreme that they name: `moments_query`: entry 1 along the first dimension is positive. `moments_key`: entry 1 along the first dimension is positive.
All inputs are finite; a program needn't handle non-finite values.
Results may differ from the reference program's by a relative error of at most 0.009.
Values may be sent and summed in bfloat16 or wider, within the bound.
No kernel may reach another device: no remote copies, remote signals or barrier semaphores. Data moves between devices by JAX's collectives and lax.ppermute only.
A program may use at most 64 MiB of HBM per device.

```python
import math
import jax
import jax.numpy as jnp
from jax import lax

D = 2048
DQ = 2048
DKV = 512
RANK = 512
TOKENS = 4096


def moment_draw(key, columns):
    first_key, second_key = jax.random.split(jax.random.fold_in(key, 7))
    position = jnp.arange(RANK, dtype=jnp.float32) / max(RANK - 1, 1)
    level = 0.1 * 10.0 ** position[:, None]
    first = jnp.clip(jax.random.normal(first_key, (RANK, columns), jnp.float32), -4.0, 4.0)
    spread = jnp.exp(jax.random.uniform(second_key, (RANK, columns), jnp.float32, math.log(0.05), math.log(0.5)))
    return jnp.stack([first * level, spread * level * level]).astype(jnp.float32)


def draw_moments_query(key, part):
    return moment_draw(key, DQ)


def draw_moments_key(key, part):
    return moment_draw(key, DKV)


def shard_levels(stream_key, shape, shards, smallest, largest):
    gain, own = 1.0, jax.random.fold_in(stream_key, 6)
    for dim, shards_of in shards:
        heights = jnp.exp(jax.random.uniform(jax.random.fold_in(own, dim), (shards_of,), jnp.float32, smallest / len(shards), largest / len(shards)))
        gain = gain * jnp.repeat(heights, shape[dim] // shards_of).reshape([-1 if axis == dim else 1 for axis in range(len(shape))])
    return gain


def scatter_about(own_key, shape, width, limit, cuts=(), kind=jnp.bfloat16):
    gain = shard_levels(own_key, shape, cuts, -0.22, 0.18) if cuts else 1.0
    drawn = jax.random.normal(own_key, shape, jnp.float32) * width * gain
    return jnp.minimum(jnp.maximum(drawn, -limit), limit).astype(kind)


def setup_inputs(seed: int = 0) -> dict:
    streams_of = jax.random.split(jax.random.key(seed), 10)
    inputs = scatter_about(streams_of[0], (TOKENS, D), 1.0, 6.0, ((0, 16),))
    cot_query = scatter_about(streams_of[1], (TOKENS, DQ), (1.0 / (TOKENS ** 0.5)), 0.09375, ((0, 16), (1, 2)))
    cot_key = scatter_about(streams_of[2], (TOKENS, DKV), (1.0 / (TOKENS ** 0.5)), 0.09375, ((0, 16), (1, 2)))
    basis_query = scatter_about(streams_of[3], (D, RANK), D ** -0.5, 0.125, ((0, 4),))
    basis_key = scatter_about(streams_of[4], (D, RANK), D ** -0.5, 0.125, ((0, 4),))
    weight_query = scatter_about(streams_of[5], (D, DQ), D ** -0.5, 0.125, ((0, 4), (1, 2)), jnp.float32)
    weight_key = scatter_about(streams_of[6], (D, DKV), D ** -0.5, 0.125, ((0, 4), (1, 2)), jnp.float32)
    moments_query = draw_moments_query(jax.random.fold_in(streams_of[9], 71), 0)
    moments_key = draw_moments_key(jax.random.fold_in(streams_of[9], 71), 0)
    return dict(inputs=inputs, cot_query=cot_query, cot_key=cot_key, basis_query=basis_query, basis_key=basis_key, weight_query=weight_query, weight_key=weight_key, moments_query=moments_query, moments_key=moments_key)


def reference(inputs, cot_query, cot_key, basis_query, basis_key, weight_query, weight_key, moments_query, moments_key):
    span = math.gcd(TOKENS, 8192)
    blocks = TOKENS // span
    in_blocks = inputs.reshape(blocks, span, D)
    query_blocks = cot_query.reshape(blocks, span, DQ)
    key_blocks = cot_key.reshape(blocks, span, DKV)

    def add_block(totals, pieces):
        rows, c_query, c_key = pieces
        rows = rows.astype(jnp.float32)
        grad_q = jnp.dot(rows.T, c_query.astype(jnp.float32), precision=lax.Precision.HIGHEST, preferred_element_type=jnp.float32)
        grad_k = jnp.dot(rows.T, c_key.astype(jnp.float32), precision=lax.Precision.HIGHEST, preferred_element_type=jnp.float32)
        return ((totals[0] + grad_q, totals[1] + grad_k), None)
    start = (jnp.zeros((D, DQ), jnp.float32), jnp.zeros((D, DKV), jnp.float32))
    (grad_query, grad_key), unused = lax.scan(add_block, start, (in_blocks, query_blocks, key_blocks))

    def update(grad, basis, weight, moments):
        low = jnp.dot(basis.astype(jnp.float32).T, grad, precision=lax.Precision.HIGHEST, preferred_element_type=jnp.float32)
        first = 0.9 * moments[0] + 0.1 * low
        second = 0.95 * moments[1] + 0.05 * low * low
        normed = first / (jnp.sqrt(second) + 1e-08)
        scale = lax.rsqrt(jnp.mean(normed * normed) + 1e-06)
        direction = normed.astype(jnp.bfloat16)
        step = scale * jnp.dot(basis, direction, preferred_element_type=jnp.float32)
        new_weight = weight - 0.02 * step
        return (step, new_weight, new_weight.astype(jnp.bfloat16), jnp.stack([first, second]))
    step_q, weight_q, copy_q, moments_q = update(grad_query, basis_query, weight_query, moments_query)
    step_k, weight_k, copy_k, moments_k = update(grad_key, basis_key, weight_key, moments_key)
    return (step_q, step_k, weight_q, weight_k, copy_q, copy_k, moments_q, moments_k)
```

```python
import functools

import jax
import jax.numpy as jnp
from jax import lax
from jax.experimental import pallas as pl
from jax.experimental.pallas import tpu as pltpu
from jax.sharding import PartitionSpec as P

BF = jnp.bfloat16
F32 = jnp.float32


def contract(left, right):
    return lax.dot_general(left, right, (((0,), (0,)), ((), ())), preferred_element_type=F32)


def xor_swap(value, axis, bit):
    size = lax.axis_size(axis)
    return lax.ppermute(value, axis, [(i, i ^ bit) for i in range(size)])


def gather_all(value, axis):
    copies = jnp.broadcast_to(value[None], (lax.axis_size(axis), *value.shape))
    return lax.all_to_all(copies, axis, 0, 0, tiled=True)


def spread_weights(quarter):
    held = quarter[None]
    bit = lax.axis_size("fs") // 2
    while bit:
        held = jnp.concatenate([held, xor_swap(held, "fs", bit)], axis=0)
        bit //= 2
    rest = held[1:]
    if lax.axis_size("rep") != 4:
        return [[rest]] + [[xor_swap(rest, "rep", i)] for i in range(1, lax.axis_size("rep"))]
    half = rest.shape[2] // 2
    from_one = xor_swap(rest, "rep", 1)
    from_two = xor_swap(rest, "rep", 2)
    left = xor_swap(from_one[:, :, :half], "rep", 2)
    right = xor_swap(from_two[:, :, half:], "rep", 1)
    return [[rest], [from_one], [from_two], [left, right]]


def rel_blocks(n_f):
    held, bit = [0], n_f // 2
    while bit:
        held = held + [i ^ bit for i in held]
        bit //= 2
    return held


def finish_kernel(n_r, counts, where_ref, scale_ref, mine_ref, other_ref, dq_ref, dk_ref, wq_ref, wk_ref, *refs):
    pieces, outs = refs[:-6], refs[-6:]
    step_q, step_k, new_q, new_k, copy_q, copy_k = outs
    j = pl.program_id(0)
    h = mine_ref.shape[2]
    r = where_ref[0]
    query_mine = where_ref[1] == 0
    cols = dq_ref.shape[1]

    def products(i):
        at = jnp.bitwise_xor(r, i)
        mine, other = mine_ref[at, 0], other_ref[at, 0]
        q = jnp.where(query_mine, mine, other)
        k = jnp.where(query_mine, other, mine)
        q = jnp.dot(q, dq_ref[...], preferred_element_type=F32)
        k = jnp.dot(k, dk_ref[...], preferred_element_type=F32)
        return pl.ds(pl.multiple_of(at * h, h), h), scale_ref[0] * q, scale_ref[1] * k

    @pl.when(j == 0)
    def _():
        for i in range(n_r):
            rows, q, k = products(i)
            step_q[rows, :] = q
            step_k[rows, :] = k
            q = wq_ref[rows, :] - 0.02 * q
            k = wk_ref[rows, :] - 0.02 * k
            new_q[rows, :] = q
            new_k[rows, :] = k
            copy_q[rows, :] = q.astype(BF)
            copy_k[rows, :] = k.astype(BF)

    @pl.when(j != 0)
    def _():
        first = 0
        for i in range(n_r):
            rows, q, k = products(i)
            got = pieces[first : first + counts[i]]
            first += counts[i]
            w = [g[0] for g in got]
            w = (w[0] if len(w) == 1 else jnp.concatenate(w, axis=1)).astype(F32)
            copy_q[rows, :] = (w[:, :cols] - 0.02 * q).astype(BF)
            copy_k[rows, :] = (w[:, cols:] - 0.02 * k).astype(BF)


def finish(where, scales, mine, other, dir_q, dir_k, weight_q, weight_k, pieces):
    n_r, n_f, h, rank = mine.shape
    counts = tuple(len(p) for p in pieces)
    flat = [a for p in pieces for a in p]
    rows = h * n_r
    cols_q, cols_k = dir_q.shape[1], dir_k.shape[1]
    whole = lambda a: pl.BlockSpec(a.shape, lambda j, w: (0,) * a.ndim)
    fixed = lambda shape: pl.BlockSpec(shape, lambda j, w: (0, 0))
    rel = lambda shape: pl.BlockSpec(shape, lambda j, w: (w[2 + j], 0))
    basis = pl.BlockSpec((n_r, 1, h, rank), lambda j, w: (0, w[2 + j], 0, 0))
    piece = lambda a: pl.BlockSpec((1, *a.shape[1:]), lambda j, w: (jnp.maximum(j - 1, 0), 0, 0))
    return pl.pallas_call(
        functools.partial(finish_kernel, n_r, counts),
        grid_spec=pltpu.PrefetchScalarGridSpec(
            num_scalar_prefetch=1,
            grid=(n_f,),
            in_specs=[
                pl.BlockSpec(memory_space=pltpu.SMEM),
                basis,
                basis,
                whole(dir_q),
                whole(dir_k),
                whole(weight_q),
                whole(weight_k),
                *[piece(a) for a in flat],
            ],
            out_specs=[
                fixed((rows, cols_q)),
                fixed((rows, cols_k)),
                fixed((rows, cols_q)),
                fixed((rows, cols_k)),
                rel((rows, cols_q)),
                rel((rows, cols_k)),
            ],
        ),
        out_shape=[
            jax.ShapeDtypeStruct((rows, cols_q), F32),
            jax.ShapeDtypeStruct((rows, cols_k), F32),
            jax.ShapeDtypeStruct((rows, cols_q), F32),
            jax.ShapeDtypeStruct((rows, cols_k), F32),
            jax.ShapeDtypeStruct((rows * n_f, cols_q), BF),
            jax.ShapeDtypeStruct((rows * n_f, cols_k), BF),
        ],
        compiler_params=pltpu.CompilerParams(vmem_limit_bytes=56 * 2**20),
        name="finish",
    )(where, scales, mine, other, dir_q, dir_k, weight_q, weight_k, *flat)


def update(first, second, low):
    first = 0.9 * first + 0.1 * low
    second = 0.95 * second + 0.05 * low * low
    return first, second, (first / (jnp.sqrt(second) + 1e-08)).astype(BF)


def on_device(
    inputs,
    cot_query,
    cot_key,
    basis_query,
    basis_key,
    weight_query,
    weight_key,
    moments_query,
    moments_key,
):
    n_f, n_r = lax.axis_size("fs"), lax.axis_size("rep")
    z, r, t = lax.axis_index("fs"), lax.axis_index("rep"), lax.axis_index("tp")
    tokens, d = inputs.shape
    own_rows, rank = basis_query.shape
    h = own_rows // n_r
    cols_q, cols_k = cot_query.shape[1], cot_key.shape[1]
    low_h = rank // (n_f * n_r)

    basis = jnp.where(t == 0, basis_query, basis_key)
    basis = lax.dynamic_slice_in_dim(basis, r * h, h, 0)
    basis = gather_all(gather_all(basis, "fs"), "rep")

    quarter = jnp.concatenate(
        [
            lax.dynamic_slice_in_dim(weight_query, r * h, h, 0).astype(BF),
            lax.dynamic_slice_in_dim(weight_key, r * h, h, 0).astype(BF),
        ],
        axis=1,
    )
    pieces = spread_weights(quarter)
    other_basis = xor_swap(basis, "tp", 1)

    token = jnp.dot(
        inputs, basis.transpose(1, 0, 2, 3).reshape(d, rank), preferred_element_type=F32
    ).astype(BF)
    other_token = xor_swap(token, "tp", 1)
    token_q = jnp.where(t == 0, token, other_token)
    token_k = jnp.where(t == 0, other_token, token)
    low = jnp.concatenate([contract(token_q, cot_query), contract(token_k, cot_key)], axis=1)
    low = low.astype(BF).reshape(n_f, n_r, low_h, cols_q + cols_k).transpose(1, 0, 2, 3)
    low = jnp.sum(lax.all_to_all(low, "rep", 0, 0, tiled=True).astype(F32), axis=0).astype(BF)
    low = jnp.sum(lax.all_to_all(low, "fs", 0, 0, tiled=True).astype(F32), axis=0).astype(BF)

    moments = [
        jnp.concatenate([moments_query[i], moments_key[i]], axis=1) for i in range(2)
    ]
    mine = [lax.dynamic_slice_in_dim(m, r * low_h, low_h, 0) for m in moments]
    direction = update(*mine, low.astype(F32))[2]
    rows = gather_all(direction, "fs")
    here = lax.broadcasted_iota(jnp.int32, rows.shape, 0) == z
    rows = gather_all(jnp.where(here, low[None], rows), "rep")
    rows = rows.transpose(1, 0, 2, 3).reshape(n_f, rank // n_f, cols_q + cols_k)
    low = lax.dynamic_index_in_dim(rows, z, 0, keepdims=False).astype(F32)
    first, second, direction = update(*moments, low)
    here = lax.broadcasted_iota(jnp.int32, rows.shape, 0) == z
    rows = jnp.where(here, direction[None], rows).reshape(rank, cols_q + cols_k)
    dir_q, dir_k = rows[:, :cols_q], rows[:, cols_q:]
    totals = jnp.stack([jnp.sum(jnp.square(dir_q.astype(F32))), jnp.sum(jnp.square(dir_k.astype(F32)))])
    totals = totals + xor_swap(totals, "tp", 1) if lax.axis_size("tp") == 2 else lax.psum(totals, "tp")
    count = jnp.array([rank * cols_q, rank * cols_k], F32) * lax.axis_size("tp")
    scales = lax.rsqrt(totals / count + 1e-06)
    new_moments = jnp.stack([first, second])

    blocks = jnp.bitwise_xor(z, jnp.array(rel_blocks(n_f), jnp.int32))
    where = jnp.concatenate([jnp.stack([r, t]).astype(jnp.int32), blocks])
    outs = finish(where, scales, basis, other_basis, dir_q, dir_k, weight_query, weight_key, pieces)
    return (*outs, new_moments[:, :, :cols_q], new_moments[:, :, cols_q:])


def solution(mesh):
    in_specs = (
        P(("fs", "rep"), None),
        P(("fs", "rep"), "tp"),
        P(("fs", "rep"), "tp"),
        P("fs", None),
        P("fs", None),
        P("fs", "tp"),
        P("fs", "tp"),
        P(None, "fs", "tp"),
        P(None, "fs", "tp"),
    )
    out_specs = (
        P("fs", "tp"),
        P("fs", "tp"),
        P("fs", "tp"),
        P("fs", "tp"),
        P(None, "tp"),
        P(None, "tp"),
        P(None, "fs", "tp"),
        P(None, "fs", "tp"),
    )
    return jax.shard_map(
        on_device, mesh=mesh, in_specs=in_specs, out_specs=out_specs, check_vma=False
    )
```

```python
import functools

import jax
import jax.numpy as jnp
from jax import lax
from jax.experimental import pallas as pl
from jax.experimental.pallas import tpu as pltpu
from jax.sharding import PartitionSpec as P


BF = jnp.bfloat16
F32 = jnp.float32
SMALL = pltpu.CompilerParams(vmem_limit_bytes=16 * 2**20)
LARGE = pltpu.CompilerParams(vmem_limit_bytes=30 * 2**20)


def whole(a):
    shape = getattr(a, "shape", a)
    return pl.BlockSpec(tuple(shape), lambda *_: (0,) * len(shape))


def contract(left, right):
    return lax.dot_general(left, right, (((0,), (0,)), ((), ())), preferred_element_type=F32)


def xor_swap(value, axis, bit):
    size = lax.axis_size(axis)
    return lax.ppermute(value, axis, [(i, i ^ bit) for i in range(size)])


def exchange(value, axis):
    return lax.all_to_all(value, axis, 0, 0, tiled=True)


def spread(own):
    own = own[None]
    rest, rels = None, []
    bit = lax.axis_size("fs") // 2
    while bit:
        near = xor_swap(own, "fs", bit)
        if rest is None:
            rest, rels = near, [bit]
        elif bit > 1:
            far = xor_swap(rest, "fs", bit)
            rest = jnp.concatenate([rest, near, far], axis=0)
            rels = rels + [bit] + [i ^ bit for i in rels]
        else:
            far = xor_swap(rest, "fs", bit)
            return [([bit], near), (rels, rest), ([i ^ bit for i in rels], far)]
        bit //= 2
    return [(rels, rest)]


def parity(r):
    return jnp.bitwise_xor(jnp.bitwise_and(r, 1), jnp.right_shift(r, 1))


def share(r):
    return (2 * parity(r), 2) if lax.axis_size("rep") == 4 else (r, 1)


def spread_planes(own):
    n_r = lax.axis_size("rep")
    pieces = []
    for rels, got in spread(own):
        pieces.append((rels, got, lambda r: share(r)[0]))
        if n_r == 4:
            h = got.shape[1] // 2
            near = xor_swap(got[:, :h], "rep", 1)
            pieces.append((rels, near, lambda r: 2 - 2 * parity(r)))
            near = xor_swap(got[:, h:], "rep", 2)
            pieces.append((rels, near, lambda r: 3 - 2 * parity(r)))
        else:
            for i in range(1, n_r):
                near = xor_swap(got, "rep", i)
                pieces.append((rels, near, lambda r, i=i: jnp.bitwise_xor(r, i)))
    return pieces


def token_kernel(rels, z_ref, r_ref, x_ref, own_ref, *refs):
    parts, (basis_ref, token_ref), (x_vmem, sem) = refs[:-4], refs[-4:-2], refs[-2:]
    load = pltpu.make_async_copy(x_ref, x_vmem, sem)
    load.start()
    z = z_ref[0]
    rows = own_ref.shape[0]
    basis_ref[pl.ds(pl.multiple_of(z * rows, rows), rows), :] = own_ref[...]
    for (rel, first), part in zip(rels, parts):
        size = part.shape[1]
        for j, rel_j in enumerate(rel):
            at = jnp.bitwise_xor(z, rel_j) * rows + first(r_ref[0]) * (rows // lax.axis_size("rep"))
            basis_ref[pl.ds(pl.multiple_of(at, 16), size), :] = part[j]
    load.wait()
    token_ref[...] = jnp.dot(x_vmem[...], basis_ref[...], preferred_element_type=F32).astype(BF)


def tokens(z, r, x, own, parts):
    return pl.pallas_call(
        functools.partial(token_kernel, tuple((tuple(rel), first) for rel, _, first in parts)),
        in_specs=[pl.BlockSpec(memory_space=pltpu.SMEM)] * 2
        + [pl.BlockSpec(memory_space=pltpu.HBM), whole(own)]
        + [whole(p) for _, p, _ in parts],
        out_specs=[whole((x.shape[1], own.shape[1])), whole((x.shape[0], own.shape[1]))],
        grid=(1,),
        out_shape=[
            jax.ShapeDtypeStruct((x.shape[1], own.shape[1]), BF),
            jax.ShapeDtypeStruct((x.shape[0], own.shape[1]), BF),
        ],
        scratch_shapes=[pltpu.VMEM(x.shape, BF), pltpu.SemaphoreType.DMA],
        compiler_params=SMALL,
        name="tokens",
    )(z, r, x, own, *[p for _, p, _ in parts])


def terms_kernel(t_ref, mine_ref, other_ref, cq_ref, ck_ref, out_ref):
    n_r, n_f, rows, _ = out_ref.shape
    cols_q = cq_ref.shape[1]
    query_mine = t_ref[0] == 0
    mine, other = mine_ref[...], other_ref[...]
    q = contract(jnp.where(query_mine, mine, other), cq_ref[...]).astype(BF)
    k = contract(jnp.where(query_mine, other, mine), ck_ref[...]).astype(BF)
    for j in range(n_f):
        for i in range(n_r):
            at = (j * n_r + i) * rows
            out_ref[i, j, :, :cols_q] = q[at : at + rows]
            out_ref[i, j, :, cols_q:] = k[at : at + rows]


def terms(t, mine, other, cot_q, cot_k):
    n_f, n_r = lax.axis_size("fs"), lax.axis_size("rep")
    shape = (n_r, n_f, mine.shape[1] // (n_f * n_r), cot_q.shape[1] + cot_k.shape[1])
    return pl.pallas_call(
        terms_kernel,
        in_specs=[pl.BlockSpec(memory_space=pltpu.SMEM)]
        + [whole(a) for a in (mine, other, cot_q, cot_k)],
        out_specs=whole(shape),
        grid=(1,),
        out_shape=jax.ShapeDtypeStruct(shape, BF),
        compiler_params=SMALL,
        name="terms",
    )(t, mine, other, cot_q, cot_k)


def sum_kernel(in_ref, out_ref):
    total = in_ref[0].astype(F32)
    for i in range(1, in_ref.shape[0]):
        total = total + in_ref[i].astype(F32)
    out_ref[...] = total.astype(BF)


def sum_first(value):
    return pl.pallas_call(
        sum_kernel,
        in_specs=[whole(value)],
        out_specs=whole(value.shape[1:]),
        grid=(1,),
        out_shape=jax.ShapeDtypeStruct(value.shape[1:], BF),
        compiler_params=SMALL,
        name="sum_first",
    )(value)


def moment_update(first, second, low):
    first = 0.9 * first + 0.1 * low
    second = 0.95 * second + 0.05 * low * low
    return first, second, first / (jnp.sqrt(second) + 1e-08)


def piece_kernel(got_ref, mq_ref, mk_ref, low_ref, out_ref):
    cols_q = mq_ref.shape[2]
    total = got_ref[0].astype(F32)
    for i in range(1, got_ref.shape[0]):
        total = total + got_ref[i].astype(F32)
    low = total.astype(BF)
    low_ref[...] = low
    low = low.astype(F32)
    q = moment_update(mq_ref[0], mq_ref[1], low[:, :cols_q])[2].astype(BF)
    k = moment_update(mk_ref[0], mk_ref[1], low[:, cols_q:])[2].astype(BF)
    for i in range(out_ref.shape[0]):
        out_ref[i, :, :cols_q] = q
        out_ref[i, :, cols_q:] = k


def piece(r, got, moments_q, moments_k):
    n_f, rows, cols = got.shape
    moments_q = lax.dynamic_slice_in_dim(moments_q, r * rows, rows, 1)
    moments_k = lax.dynamic_slice_in_dim(moments_k, r * rows, rows, 1)
    return pl.pallas_call(
        piece_kernel,
        in_specs=[whole(got), whole(moments_q), whole(moments_k)],
        out_specs=[whole((rows, cols)), whole((n_f, rows, cols))],
        grid=(1,),
        out_shape=[
            jax.ShapeDtypeStruct((rows, cols), BF),
            jax.ShapeDtypeStruct((n_f, rows, cols), BF),
        ],
        compiler_params=SMALL,
        name="piece",
    )(got, moments_q, moments_k)


def plane_kernel(z_ref, got_ref, low_ref, out_ref):
    for i in range(out_ref.shape[0]):
        out_ref[i] = got_ref[...]
        out_ref[i, z_ref[0]] = low_ref[...]


def plane(z, got, low):
    return pl.pallas_call(
        plane_kernel,
        in_specs=[pl.BlockSpec(memory_space=pltpu.SMEM), whole(got), whole(low)],
        out_specs=whole((lax.axis_size("rep"), *got.shape)),
        grid=(1,),
        out_shape=jax.ShapeDtypeStruct((lax.axis_size("rep"), *got.shape), BF),
        compiler_params=SMALL,
        name="plane",
    )(z, got, low)


def squares(value):
    rows, cols = value.shape
    total = jnp.sum(jnp.square(value).reshape(rows // 8, 8, cols), axis=0)
    parts = [total[:, i : i + 128] for i in range(0, cols, 128)]
    return functools.reduce(jnp.add, parts)


def directions_kernel(z_ref, got_ref, mq_ref, mk_ref, nq_ref, nk_ref, dq_ref, dk_ref, sums_ref):
    n_r, n_f, rows, _ = got_ref.shape
    cols_q = mq_ref.shape[2]
    z = z_ref[0]
    own = n_r * rows
    for j in range(n_f):
        got = jnp.concatenate([got_ref[i, j] for i in range(n_r)], axis=0)
        dq_ref[j * own : (j + 1) * own, :] = got[:, :cols_q]
        dk_ref[j * own : (j + 1) * own, :] = got[:, cols_q:]
    low = jnp.concatenate([got_ref[i, z] for i in range(n_r)], axis=0).astype(F32)
    q = moment_update(mq_ref[0], mq_ref[1], low[:, :cols_q])
    k = moment_update(mk_ref[0], mk_ref[1], low[:, cols_q:])
    nq_ref[0], nq_ref[1] = q[0], q[1]
    nk_ref[0], nk_ref[1] = k[0], k[1]
    at = pl.ds(pl.multiple_of(z * own, own), own)
    dq_ref[at, :] = q[2].astype(BF)
    dk_ref[at, :] = k[2].astype(BF)
    sums_ref[:8, :] = squares(dq_ref[...].astype(F32))
    sums_ref[8:, :] = squares(dk_ref[...].astype(F32))


def directions(z, got, moments_q, moments_k):
    n_r, n_f, rows, _ = got.shape
    rank = n_r * n_f * rows
    return pl.pallas_call(
        directions_kernel,
        in_specs=[pl.BlockSpec(memory_space=pltpu.SMEM), whole(got), whole(moments_q), whole(moments_k)],
        out_specs=[
            whole(moments_q),
            whole(moments_k),
            whole((rank, moments_q.shape[2])),
            whole((rank, moments_k.shape[2])),
            whole((16, 128)),
        ],
        grid=(1,),
        out_shape=[
            jax.ShapeDtypeStruct(moments_q.shape, F32),
            jax.ShapeDtypeStruct(moments_k.shape, F32),
            jax.ShapeDtypeStruct((rank, moments_q.shape[2]), BF),
            jax.ShapeDtypeStruct((rank, moments_k.shape[2]), BF),
            jax.ShapeDtypeStruct((16, 128), F32),
        ],
        compiler_params=SMALL,
        name="directions",
    )(z, got, moments_q, moments_k)


def finish_kernel(
    plan, n_f, n_tp, z_ref, r_ref, t_ref, sums_ref, other_sums_ref, dq_ref, dk_ref,
    mine_ref, other_ref, wq_ref, wk_ref, *refs,
):
    n = len(plan)
    pieces, outs = refs[:n], refs[n : n + 6]
    basis, weights, held = refs[n + 6 : n + 8], refs[n + 8 : n + 10], refs[n + 10 : 2 * n + 10]
    results, copies_out = refs[2 * n + 10 : 2 * n + 14], refs[2 * n + 14 : 2 * n + 16]
    basis_sem, weight_sem, held_sem, out_sem, copy_sem = refs[2 * n + 16 :]
    z, r = z_ref[0], r_ref[0]
    rows, cols_q = wq_ref.shape
    cols_k = wk_ref.shape[1]
    rank = dq_ref.shape[0]
    h = rows // lax.axis_size("rep")
    order = [rel for rel in range(1, n_f)]
    order = [*order[:1], 0, *order[1:]]

    def block(rel):
        return pl.ds(pl.multiple_of(jnp.bitwise_xor(z, rel) * rows, rows), rows)

    def basis_load(rel, step):
        at = block(rel)
        for mat in range(2):
            for first, source in ((0, mine_ref), (1, other_ref)):

                @pl.when((t_ref[0] == 0) == (mat == first))
                def _():
                    pltpu.make_async_copy(
                        source.at[at], basis[mat].at[step], basis_sem.at[mat, step]
                    ).start()

    weight_loads = [
        pltpu.make_async_copy(source, to, weight_sem.at[i])
        for i, (source, to) in enumerate(zip((wq_ref, wk_ref), weights))
    ]
    held_loads = {}
    for i, (rels, _) in enumerate(plan):
        for j, rel in enumerate(rels):
            held_loads[i, rel] = pltpu.make_async_copy(
                pieces[i].at[j], held[i].at[j], held_sem.at[i, j]
            )
    for step, rel in enumerate(order):
        basis_load(rel, step)
        if rel == 0:
            for load in weight_loads:
                load.start()
        for i, (rels, _) in enumerate(plan):
            if rel in rels:
                held_loads[i, rel].start()

    def scale(at, cols):
        total = jnp.sum(sums_ref[at, :] + other_sums_ref[at, :], keepdims=True)
        return lax.rsqrt(total / (rank * cols * n_tp) + 1e-06)

    scales = scale(slice(0, 8), cols_q), scale(slice(8, 16), cols_k)
    directions = dq_ref, dk_ref
    stores = []
    for step, rel in enumerate(order):
        for mat in range(2):
            pltpu.make_async_copy(
                mine_ref.at[pl.ds(0, rows)], basis[mat].at[step], basis_sem.at[mat, step]
            ).wait()
        if rel == 0:
            for mat in range(2):
                product = jnp.dot(
                    basis[mat][step], directions[mat][...], preferred_element_type=F32
                )
                product = scales[mat] * product
                results[mat][...] = product
                weight_loads[mat].wait()
                new = weights[mat][...] - 0.02 * product
                results[2 + mat][...] = new
                copies_out[mat][step] = new.astype(BF)
                for i in (mat, 2 + mat):
                    store = pltpu.make_async_copy(results[i], outs[i], out_sem.at[i])
                    store.start()
                    stores.append(store)
        else:
            for i, (rels, first) in enumerate(plan):
                if rel not in rels:
                    continue
                held_loads[i, rel].wait()
                j = rels.index(rel)
                size = held[i].shape[1]
                at = pl.ds(pl.multiple_of(first(r) * h, 16), size)
                for mat in range(2):
                    part = slice(0, cols_q) if mat == 0 else slice(cols_q, cols_q + cols_k)
                    product = jnp.dot(
                        basis[mat][step, at, :], directions[mat][...], preferred_element_type=F32
                    )
                    new = held[i][j, :, part].astype(F32) - (0.02 * scales[mat]) * product
                    copies_out[mat][step, at, :] = new.astype(BF)
        for mat in range(2):
            store = pltpu.make_async_copy(
                copies_out[mat].at[step], outs[4 + mat].at[block(rel)], copy_sem.at[mat, step]
            )
            store.start()
            stores.append(store)
    for store in stores:
        store.wait()


def finish(z, r, t, sums, other_sums, dir_q, dir_k, mine, other, weight_q, weight_k, pieces):
    n_f, n_tp = lax.axis_size("fs"), lax.axis_size("tp")
    rows, cols_q = weight_q.shape
    cols_k = weight_k.shape[1]
    rank = mine.shape[1]
    plan = tuple((tuple(rels), first) for rels, _, first in pieces)
    arrays = [a for _, a, _ in pieces]
    hbm = pl.BlockSpec(memory_space=pltpu.HBM)
    smem = pl.BlockSpec(memory_space=pltpu.SMEM)
    shapes = [
        ((rows, cols_q), F32),
        ((rows, cols_k), F32),
        ((rows, cols_q), F32),
        ((rows, cols_k), F32),
        ((rows * n_f, cols_q), BF),
        ((rows * n_f, cols_k), BF),
    ]
    count = max(len(rels) for rels, _ in plan)
    return pl.pallas_call(
        functools.partial(finish_kernel, plan, n_f, n_tp),
        grid=(1,),
        in_specs=[smem] * 3
        + [whole(a) for a in (sums, other_sums, dir_q, dir_k)]
        + [hbm] * (4 + len(arrays)),
        out_specs=[hbm] * 6,
        out_shape=[jax.ShapeDtypeStruct(*s) for s in shapes],
        scratch_shapes=[
            *[pltpu.VMEM((n_f, rows, rank), BF)] * 2,
            pltpu.VMEM((rows, cols_q), F32),
            pltpu.VMEM((rows, cols_k), F32),
            *[pltpu.VMEM(a.shape, BF) for a in arrays],
            *[pltpu.VMEM(*s) for s in shapes[:4]],
            pltpu.VMEM((n_f, rows, cols_q), BF),
            pltpu.VMEM((n_f, rows, cols_k), BF),
            pltpu.SemaphoreType.DMA((2, n_f)),
            pltpu.SemaphoreType.DMA((2,)),
            pltpu.SemaphoreType.DMA((len(arrays), count)),
            pltpu.SemaphoreType.DMA((4,)),
            pltpu.SemaphoreType.DMA((2, n_f)),
        ],
        compiler_params=LARGE,
        name="finish",
    )(z, r, t, sums, other_sums, dir_q, dir_k, mine, other, weight_q, weight_k, *arrays)


def on_device(
    inputs,
    cot_query,
    cot_key,
    basis_query,
    basis_key,
    weight_query,
    weight_key,
    moments_query,
    moments_key,
):
    n_r = lax.axis_size("rep")
    z, r, t = lax.axis_index("fs"), lax.axis_index("rep"), lax.axis_index("tp")
    own_rows, _ = basis_query.shape
    h = own_rows // n_r
    at_z, at_r, at_t = (i.astype(jnp.int32)[None] for i in (z, r, t))
    first, count = share(r)

    own = jnp.where(t == 0, basis_query, basis_key)
    parts = spread_planes(lax.dynamic_slice_in_dim(own, first * h, count * h, 0))

    mine = [
        lax.dynamic_slice_in_dim(w, first * h, count * h, 0).astype(BF)
        for w in (weight_query, weight_key)
    ]
    pieces = spread_planes(jnp.concatenate(mine, axis=1))

    basis, token = tokens(at_z, at_r, inputs, own, parts)
    other_token = xor_swap(token, "tp", 1)
    other_basis = xor_swap(basis, "tp", 1)
    low = exchange(terms(at_t, token, other_token, cot_query, cot_key), "rep")
    low = exchange(sum_first(low), "fs")
    low, rows = piece(r, low, moments_query, moments_key)
    rows = plane(at_z, exchange(rows, "fs"), low)
    rows = exchange(rows, "rep")
    new_q, new_k, dir_q, dir_k, sums = directions(at_z, rows, moments_query, moments_key)
    other_sums = xor_swap(sums, "tp", 1)
    outs = finish(
        at_z, at_r, at_t, sums, other_sums, dir_q, dir_k, basis, other_basis,
        weight_query, weight_key, pieces,
    )
    return (*outs, new_q, new_k)


def solution(mesh):
    in_specs = (
        P(("fs", "rep"), None),
        P(("fs", "rep"), "tp"),
        P(("fs", "rep"), "tp"),
        P("fs", None),
        P("fs", None),
        P("fs", "tp"),
        P("fs", "tp"),
        P(None, "fs", "tp"),
        P(None, "fs", "tp"),
    )
    out_specs = (
        P("fs", "tp"),
        P("fs", "tp"),
        P("fs", "tp"),
        P("fs", "tp"),
        P(None, "tp"),
        P(None, "tp"),
        P(None, "fs", "tp"),
        P(None, "fs", "tp"),
    )

    return jax.shard_map(
        on_device, mesh=mesh, in_specs=in_specs, out_specs=out_specs, check_vma=False
    )
```

```python
import functools

import jax
import jax.numpy as jnp
from jax import lax
from jax.experimental import pallas as pl
from jax.experimental.pallas import tpu as pltpu
from jax.sharding import PartitionSpec as P


BF = jnp.bfloat16
F32 = jnp.float32
SMALL = pltpu.CompilerParams(vmem_limit_bytes=12 * 2**20)
LARGE = pltpu.CompilerParams(vmem_limit_bytes=28 * 2**20)


def whole(a):
    shape = getattr(a, "shape", a)
    return pl.BlockSpec(tuple(shape), lambda *_: (0,) * len(shape))


in_space = pltpu.with_memory_space_constraint


def contract(left, right):
    return lax.dot_general(left, right, (((0,), (0,)), ((), ())), preferred_element_type=F32)


def xor_swap(value, axis, bit):
    size = lax.axis_size(axis)
    return lax.ppermute(value, axis, [(i, i ^ bit) for i in range(size)])


def exchange(value, axis):
    return lax.all_to_all(value, axis, 0, 0, tiled=True)


def spread(own):
    own = own[None]
    rest, rels = None, []
    bit = lax.axis_size("fs") // 2
    while bit:
        near = xor_swap(own, "fs", bit)
        if rest is None:
            rest, rels = near, [bit]
        elif bit > 1:
            far = xor_swap(rest, "fs", bit)
            rest = jnp.concatenate([rest, near, far], axis=0)
            rels = rels + [bit] + [i ^ bit for i in rels]
        else:
            far = xor_swap(rest, "fs", bit)
            return [([bit], near), (rels, rest), ([i ^ bit for i in rels], far)]
        bit //= 2
    return [(rels, rest)]


def parity(r):
    return jnp.bitwise_xor(jnp.bitwise_and(r, 1), jnp.right_shift(r, 1))


def share(r):
    return (2 * parity(r), 2) if lax.axis_size("rep") == 4 else (r, 1)


def spread_planes(own):
    n_r = lax.axis_size("rep")
    pieces = []
    for m, part in enumerate(own):
        for n, (rels, got) in enumerate(spread(part)):
            pieces.append((rels, got, lambda r, m=m: share(r)[0] + m, n))
            if n_r != 4:
                for i in range(1, n_r):
                    near = xor_swap(got, "rep", i)
                    pieces.append((rels, near, lambda r, i=i: jnp.bitwise_xor(r, i), n))
            elif len(own) == 2:
                near = xor_swap(got, "rep", 1 + m)
                pieces.append((rels, near, lambda r, m=m: 2 + m - 2 * parity(r), n))
            else:
                h = got.shape[1] // 2
                for i, half in enumerate((got[:, :h], got[:, h:])):
                    near = xor_swap(half, "rep", 1 + i)
                    pieces.append((rels, near, lambda r, i=i: 2 + i - 2 * parity(r), n))
    return pieces


def spread_basis(basis_q, basis_k, r, t):
    n_f, n_r = lax.axis_size("fs"), lax.axis_size("rep")
    h = basis_q.shape[0] // n_r

    def rows(first, count):
        mine = (lax.dynamic_slice_in_dim(b, first * h, count * h, 0) for b in (basis_q, basis_k))
        return jnp.where(t == 0, *mine)

    first, count = share(r)
    if n_f != 4 or n_r != 4:
        return spread_planes([rows(first, count)])
    two = xor_swap(rows(r, 1)[None], "fs", 2)
    one = xor_swap(rows(first, count)[None], "fs", 1)
    three = xor_swap(two, "fs", 1)
    pieces = [([1], one, lambda r: share(r)[0], 0)]
    for i, half in enumerate((one[:, :h], one[:, h:])):
        near = xor_swap(half, "rep", 1 + i)
        pieces.append(([1], near, lambda r, i=i: 2 + i - 2 * parity(r), 0))
    for rel, got in ((2, two), (3, three)):
        pieces.append(([rel], got, lambda r: r, rel - 1))
        for i in range(1, n_r):
            near = xor_swap(got, "rep", i)
            pieces.append(([rel], near, lambda r, i=i: jnp.bitwise_xor(r, i), rel - 1))
    return pieces


def token_kernel(rels, z_ref, r_ref, t_ref, x_ref, own_q_ref, own_k_ref, *refs):
    parts, (basis_ref, token_ref) = refs[: len(rels)], refs[len(rels) : len(rels) + 2]
    x_vmem, basis_vmem, x_sem, own_sem, sems, out_sem = refs[len(rels) + 2 :]
    x_load = pltpu.make_async_copy(x_ref, x_vmem, x_sem)
    x_load.start()
    z = z_ref[0]
    rows = own_q_ref.shape[0]
    own_at = pl.ds(pl.multiple_of(z * rows, rows), rows)
    for query, source in ((True, own_q_ref), (False, own_k_ref)):

        @pl.when((t_ref[0] == 0) == query)
        def _():
            pltpu.make_async_copy(source, basis_vmem.at[own_at], own_sem).start()

    loads = []
    for n, ((rel, first), part) in enumerate(zip(rels, parts)):
        for j, rel_j in enumerate(rel):
            at = jnp.bitwise_xor(z, rel_j) * rows + first(r_ref[0]) * (rows // lax.axis_size("rep"))
            at = pl.ds(pl.multiple_of(at, 16), part.shape[1])
            loads.append(pltpu.make_async_copy(part.at[j], basis_vmem.at[at], sems.at[n, j]))
            loads[-1].start()
    x_load.wait()
    pltpu.make_async_copy(own_q_ref, basis_vmem.at[own_at], own_sem).wait()
    for load in loads:
        load.wait()
    store = pltpu.make_async_copy(basis_vmem, basis_ref, out_sem)
    store.start()
    token_ref[...] = jnp.dot(x_vmem[...], basis_vmem[...], preferred_element_type=F32).astype(BF)
    store.wait()


def tokens(z, r, t, x, own_q, own_k, parts):
    shape = (x.shape[1], own_q.shape[1])
    hbm = pl.BlockSpec(memory_space=pltpu.HBM)
    token = (x.shape[0], own_q.shape[1])
    sources = (x, own_q, own_k, *[p for _, p, _, _ in parts])
    return pl.pallas_call(
        functools.partial(token_kernel, tuple((tuple(rel), first) for rel, _, first, _ in parts)),
        in_specs=[pl.BlockSpec(memory_space=pltpu.SMEM)] * 3 + [hbm] * len(sources),
        out_specs=[hbm, whole(token)],
        grid=(1,),
        out_shape=[pltpu.HBM(shape, BF), pltpu.VMEM(token, BF)],
        scratch_shapes=[
            pltpu.VMEM(x.shape, BF),
            pltpu.VMEM(shape, BF),
            pltpu.SemaphoreType.DMA,
            pltpu.SemaphoreType.DMA,
            pltpu.SemaphoreType.DMA((len(parts), max(len(rel) for rel, _, _, _ in parts))),
            pltpu.SemaphoreType.DMA,
        ],
        compiler_params=SMALL,
        name="tokens",
    )(z, r, t, *[in_space(a, pltpu.HBM) for a in sources[:3]], *sources[3:])


def terms_kernel(t_ref, mine_ref, other_ref, cq_ref, ck_ref, out_ref):
    n_r, n_f, rows, _ = out_ref.shape
    cols_q = cq_ref.shape[1]
    query_mine = t_ref[0] == 0
    mine, other = mine_ref[...], other_ref[...]
    q = contract(jnp.where(query_mine, mine, other), cq_ref[...]).astype(BF)
    k = contract(jnp.where(query_mine, other, mine), ck_ref[...]).astype(BF)
    for j in range(n_f):
        for i in range(n_r):
            at = (j * n_r + i) * rows
            out_ref[i, j, :, :cols_q] = q[at : at + rows]
            out_ref[i, j, :, cols_q:] = k[at : at + rows]


def terms(t, mine, other, cot_q, cot_k):
    n_f, n_r = lax.axis_size("fs"), lax.axis_size("rep")
    shape = (n_r, n_f, mine.shape[1] // (n_f * n_r), cot_q.shape[1] + cot_k.shape[1])
    return pl.pallas_call(
        terms_kernel,
        in_specs=[pl.BlockSpec(memory_space=pltpu.SMEM)]
        + [whole(a) for a in (mine, other, cot_q, cot_k)],
        out_specs=whole(shape),
        grid=(1,),
        out_shape=pltpu.HBM(shape, BF),
        compiler_params=SMALL,
        name="terms",
    )(t, mine, other, cot_q, cot_k)


def sum_kernel(in_ref, out_ref):
    total = in_ref[0].astype(F32)
    for i in range(1, in_ref.shape[0]):
        total = total + in_ref[i].astype(F32)
    out_ref[...] = total.astype(BF)


def sum_first(value):
    return pl.pallas_call(
        sum_kernel,
        in_specs=[whole(value)],
        out_specs=whole(value.shape[1:]),
        grid=(1,),
        out_shape=pltpu.HBM(value.shape[1:], BF),
        compiler_params=SMALL,
        name="sum_first",
    )(value)


def moment_update(first, second, low):
    first = 0.9 * first + 0.1 * low
    second = 0.95 * second + 0.05 * low * low
    return first, second, first / (jnp.sqrt(second) + 1e-08)


def piece_kernel(got_ref, mq_ref, mk_ref, low_ref, out_ref):
    cols_q = mq_ref.shape[2]
    total = got_ref[0].astype(F32)
    for i in range(1, got_ref.shape[0]):
        total = total + got_ref[i].astype(F32)
    low = total.astype(BF)
    low_ref[...] = low
    low = low.astype(F32)
    q = moment_update(mq_ref[0], mq_ref[1], low[:, :cols_q])[2].astype(BF)
    k = moment_update(mk_ref[0], mk_ref[1], low[:, cols_q:])[2].astype(BF)
    for i in range(out_ref.shape[0]):
        out_ref[i, :, :cols_q] = q
        out_ref[i, :, cols_q:] = k


def piece(r, got, moments_q, moments_k):
    n_f, rows, cols = got.shape
    moments_q = lax.dynamic_slice_in_dim(moments_q, r * rows, rows, 1)
    moments_k = lax.dynamic_slice_in_dim(moments_k, r * rows, rows, 1)
    return pl.pallas_call(
        piece_kernel,
        in_specs=[whole(got), whole(moments_q), whole(moments_k)],
        out_specs=[whole((rows, cols)), whole((n_f, rows, cols))],
        grid=(1,),
        out_shape=[
            jax.ShapeDtypeStruct((rows, cols), BF),
            pltpu.HBM((n_f, rows, cols), BF),
        ],
        compiler_params=SMALL,
        name="piece",
    )(got, moments_q, moments_k)


def plane_kernel(z_ref, got_ref, low_ref, out_ref):
    for i in range(out_ref.shape[0]):
        out_ref[i] = got_ref[...]
        out_ref[i, z_ref[0]] = low_ref[...]


def plane(z, got, low):
    return pl.pallas_call(
        plane_kernel,
        in_specs=[pl.BlockSpec(memory_space=pltpu.SMEM), whole(got), whole(low)],
        out_specs=whole((lax.axis_size("rep"), *got.shape)),
        grid=(1,),
        out_shape=jax.ShapeDtypeStruct((lax.axis_size("rep"), *got.shape), BF),
        compiler_params=SMALL,
        name="plane",
    )(z, got, low)


def squares(value):
    rows, cols = value.shape
    total = jnp.sum(jnp.square(value).reshape(rows // 8, 8, cols), axis=0)
    parts = [total[:, i : i + 128] for i in range(0, cols, 128)]
    return functools.reduce(jnp.add, parts)


def directions_kernel(z_ref, got_ref, mq_ref, mk_ref, nq_ref, nk_ref, dq_ref, dk_ref, sums_ref):
    n_r, n_f, rows, _ = got_ref.shape
    cols_q = mq_ref.shape[2]
    z = z_ref[0]
    own = n_r * rows
    for j in range(n_f):
        got = jnp.concatenate([got_ref[i, j] for i in range(n_r)], axis=0)
        dq_ref[j * own : (j + 1) * own, :] = got[:, :cols_q]
        dk_ref[j * own : (j + 1) * own, :] = got[:, cols_q:]
    low = jnp.concatenate([got_ref[i, z] for i in range(n_r)], axis=0).astype(F32)
    q = moment_update(mq_ref[0], mq_ref[1], low[:, :cols_q])
    k = moment_update(mk_ref[0], mk_ref[1], low[:, cols_q:])
    nq_ref[0], nq_ref[1] = q[0], q[1]
    nk_ref[0], nk_ref[1] = k[0], k[1]
    at = pl.ds(pl.multiple_of(z * own, own), own)
    dq_ref[at, :] = q[2].astype(BF)
    dk_ref[at, :] = k[2].astype(BF)
    sums_ref[:8, :] = squares(dq_ref[...].astype(F32))
    sums_ref[8:, :] = squares(dk_ref[...].astype(F32))


def directions(z, got, moments_q, moments_k):
    n_r, n_f, rows, _ = got.shape
    rank = n_r * n_f * rows
    return pl.pallas_call(
        directions_kernel,
        in_specs=[pl.BlockSpec(memory_space=pltpu.SMEM), whole(got), whole(moments_q), whole(moments_k)],
        out_specs=[
            whole(moments_q),
            whole(moments_k),
            whole((rank, moments_q.shape[2])),
            whole((rank, moments_k.shape[2])),
            whole((16, 128)),
        ],
        grid=(1,),
        out_shape=[
            jax.ShapeDtypeStruct(moments_q.shape, F32),
            jax.ShapeDtypeStruct(moments_k.shape, F32),
            pltpu.VMEM((rank, moments_q.shape[2]), BF),
            pltpu.VMEM((rank, moments_k.shape[2]), BF),
            pltpu.VMEM((16, 128), F32),
        ],
        compiler_params=SMALL,
        name="directions",
    )(z, got, moments_q, moments_k)


def gather_pieces(plan, slots, rel, r, pieces, to, sems):
    loads = []
    h = to.shape[1] // lax.axis_size("rep")
    for i, (rels, first) in enumerate(plan):
        if rel in rels:
            j = rels.index(rel)
            at = pl.ds(pl.multiple_of(first(r) * h, 16), pieces[i].shape[1])
            loads.append(
                pltpu.make_async_copy(pieces[i].at[j], to.at[slots[rel], at], sems.at[i, j])
            )
            loads[-1].start()
    return loads


def slots_of(plan):
    rels = []
    for got, _ in plan:
        rels += [rel for rel in got if rel not in rels]
    return {rel: i for i, rel in enumerate(rels)}


def plan_of(pieces):
    return tuple((tuple(rels), first) for rels, _, first, _ in pieces)


def semaphores(plan):
    return pltpu.SemaphoreType.DMA((len(plan), max(len(rels) for rels, _ in plan)))


CHUNK = 256


def finish_kernel(
    plan, n_tp, z_ref, r_ref, t_ref, sums_ref, other_sums_ref, dq_ref, dk_ref,
    mine_ref, other_ref, wq_ref, wk_ref, *refs,
):
    n = len(plan)
    pieces, outs, results, copies_out = refs[:n], refs[n : n + 6], refs[n + 6 : n + 10], refs[n + 10 : n + 12]
    bases, weights, (last, basis_sem, weight_sem, out_sem, copy_sem, sems) = (
        refs[n + 12 : n + 14], refs[n + 14 : n + 16], refs[n + 16 :]
    )
    z = z_ref[0]
    rows, cols_q = wq_ref.shape
    cols_k = wk_ref.shape[1]
    rank = dq_ref.shape[0]
    slots = slots_of(plan)
    order = [*slots]
    order = [order[0], 0, *order[1:]]

    def block(rel):
        return pl.ds(pl.multiple_of(jnp.bitwise_xor(z, rel) * rows, rows), rows)

    loads = {}
    weight_loads = [
        pltpu.make_async_copy(source, to, weight_sem.at[i])
        for i, (source, to) in enumerate(zip((wq_ref, wk_ref), weights))
    ]
    for step, rel in enumerate(order):
        for query in (True, False):

            @pl.when((t_ref[0] == 0) == query)
            def _():
                for mat, source in enumerate((mine_ref, other_ref) if query else (other_ref, mine_ref)):
                    pltpu.make_async_copy(
                        source.at[block(rel)], bases[mat].at[step], basis_sem.at[mat, step]
                    ).start()

        if rel == 0:
            for load in weight_loads:
                load.start()
        else:
            loads[rel] = gather_pieces(plan, slots, rel, r_ref[0], pieces, last, sems)

    def scale(at, cols):
        total = jnp.sum(sums_ref[at, :] + other_sums_ref[at, :], keepdims=True)
        return lax.rsqrt(total / (rank * cols * n_tp) + 1e-06)

    scales = scale(slice(0, 8), cols_q), scale(slice(8, 16), cols_k)
    directions = dq_ref, dk_ref
    stores = []

    def store(source, to, sem):
        stores.append(pltpu.make_async_copy(source, to, sem))
        stores[-1].start()

    for step, rel in enumerate(order):
        for load in loads.get(rel, []):
            load.wait()
        for mat, part in ((0, slice(0, cols_q)), (1, slice(cols_q, cols_q + cols_k))):
            pltpu.make_async_copy(
                mine_ref.at[block(rel)], bases[mat].at[step], basis_sem.at[mat, step]
            ).wait()
            if rel == 0:
                weight_loads[mat].wait()
            for top in range(0, rows, CHUNK):
                at = slice(top, min(rows, top + CHUNK))
                product = jnp.dot(
                    bases[mat][step, at], directions[mat][...], preferred_element_type=F32
                )
                if rel == 0:
                    product = scales[mat] * product
                    results[mat][at] = product
                    new = weights[mat][at] - 0.02 * product
                    results[2 + mat][at] = new
                else:
                    old = last[slots[rel], at, part]
                    new = old.astype(F32) - (0.02 * scales[mat]) * product
                copies_out[mat][step, at] = new.astype(BF)
            if rel == 0:
                store(results[mat], outs[mat], out_sem.at[mat])
                store(results[2 + mat], outs[2 + mat], out_sem.at[2 + mat])
            store(copies_out[mat].at[step], outs[4 + mat].at[block(rel)], copy_sem.at[mat, step])
    for one in stores:
        one.wait()


def finish(z, r, t, sums, other_sums, dir_q, dir_k, mine, other, weight_q, weight_k, pieces):
    n_f, n_tp = lax.axis_size("fs"), lax.axis_size("tp")
    rows, cols_q = weight_q.shape
    cols_k = weight_k.shape[1]
    rank = mine.shape[1]
    plan = plan_of(pieces)
    hbm = pl.BlockSpec(memory_space=pltpu.HBM)
    smem = pl.BlockSpec(memory_space=pltpu.SMEM)
    vmem = pl.BlockSpec(memory_space=pltpu.VMEM)
    shapes = [
        ((rows, cols_q), F32),
        ((rows, cols_k), F32),
        ((rows, cols_q), F32),
        ((rows, cols_k), F32),
        ((rows * n_f, cols_q), BF),
        ((rows * n_f, cols_k), BF),
    ]
    inside = [in_space(a, pltpu.VMEM) for a in (sums, other_sums, dir_q, dir_k)]
    outside = [
        in_space(a, pltpu.HBM) for a in (mine, other, weight_q, weight_k, *[p[1] for p in pieces])
    ]
    return pl.pallas_call(
        functools.partial(finish_kernel, plan, n_tp),
        in_specs=[smem] * 3 + [vmem] * len(inside) + [hbm] * len(outside),
        out_specs=[hbm] * 6,
        out_shape=[pltpu.HBM(*s) for s in shapes],
        scratch_shapes=[
            *[pltpu.VMEM(*s) for s in shapes[:4]],
            pltpu.VMEM((n_f, rows, cols_q), BF),
            pltpu.VMEM((n_f, rows, cols_k), BF),
            *[pltpu.VMEM((n_f, rows, rank), BF)] * 2,
            pltpu.VMEM((rows, cols_q), F32),
            pltpu.VMEM((rows, cols_k), F32),
            pltpu.VMEM((len(slots_of(plan)), rows, cols_q + cols_k), BF),
            pltpu.SemaphoreType.DMA((2, n_f)),
            pltpu.SemaphoreType.DMA((2,)),
            pltpu.SemaphoreType.DMA((4,)),
            pltpu.SemaphoreType.DMA((2, n_f)),
            semaphores(plan),
        ],
        compiler_params=LARGE,
        name="finish",
    )(z, r, t, *inside, *outside)


def on_device(
    inputs,
    cot_query,
    cot_key,
    basis_query,
    basis_key,
    weight_query,
    weight_key,
    moments_query,
    moments_key,
):
    n_r = lax.axis_size("rep")
    z, r, t = lax.axis_index("fs"), lax.axis_index("rep"), lax.axis_index("tp")
    own_rows, _ = basis_query.shape
    h = own_rows // n_r
    at_z, at_r, at_t = (i.astype(jnp.int32)[None] for i in (z, r, t))
    first, count = share(r)

    parts = spread_basis(basis_query, basis_key, r, t)

    mine = [
        jnp.concatenate(
            [
                lax.dynamic_slice_in_dim(w, (first + i) * h, h, 0).astype(BF)
                for w in (weight_query, weight_key)
            ],
            axis=1,
        )
        for i in range(count)
    ]
    pieces = spread_planes(mine)

    basis, token = tokens(at_z, at_r, at_t, inputs, basis_query, basis_key, parts)
    other_token = xor_swap(token, "tp", 1)
    other_basis = xor_swap(basis, "tp", 1)
    low = exchange(terms(at_t, token, other_token, cot_query, cot_key), "rep")
    low = exchange(sum_first(low), "fs")
    low, rows = piece(r, low, moments_query, moments_key)
    rows = plane(at_z, exchange(rows, "fs"), low)
    rows = exchange(rows, "rep")
    new_q, new_k, dir_q, dir_k, sums = directions(at_z, rows, moments_query, moments_key)
    other_sums = xor_swap(sums, "tp", 1)
    outs = finish(
        at_z, at_r, at_t, sums, other_sums, dir_q, dir_k,
        basis, other_basis, weight_query, weight_key, pieces,
    )
    return (*outs, new_q, new_k)


def solution(mesh):
    in_specs = (
        P(("fs", "rep"), None),
        P(("fs", "rep"), "tp"),
        P(("fs", "rep"), "tp"),
        P("fs", None),
        P("fs", None),
        P("fs", "tp"),
        P("fs", "tp"),
        P(None, "fs", "tp"),
        P(None, "fs", "tp"),
    )
    out_specs = (
        P("fs", "tp"),
        P("fs", "tp"),
        P("fs", "tp"),
        P("fs", "tp"),
        P(None, "tp"),
        P(None, "tp"),
        P(None, "fs", "tp"),
        P(None, "fs", "tp"),
    )

    return jax.shard_map(
        on_device, mesh=mesh, in_specs=in_specs, out_specs=out_specs, check_vma=False
    )
```

```python
import functools

import jax
import jax.numpy as jnp
from jax import lax
from jax.experimental import pallas as pl
from jax.experimental.pallas import tpu as pltpu
from jax.sharding import PartitionSpec as P


BF = jnp.bfloat16
F32 = jnp.float32
SMALL = pltpu.CompilerParams(vmem_limit_bytes=12 * 2**20)
LARGE = pltpu.CompilerParams(vmem_limit_bytes=28 * 2**20)


def whole(a):
    shape = getattr(a, "shape", a)
    return pl.BlockSpec(tuple(shape), lambda *_: (0,) * len(shape))


in_space = pltpu.with_memory_space_constraint


def contract(left, right):
    return lax.dot_general(left, right, (((0,), (0,)), ((), ())), preferred_element_type=F32)


def xor_swap(value, axis, bit):
    size = lax.axis_size(axis)
    return lax.ppermute(value, axis, [(i, i ^ bit) for i in range(size)])


def exchange(value, axis):
    return lax.all_to_all(value, axis, 0, 0, tiled=True)


def spread(own):
    own = own[None]
    rest, rels = None, []
    bit = lax.axis_size("fs") // 2
    while bit:
        near = xor_swap(own, "fs", bit)
        if rest is None:
            rest, rels = near, [bit]
        elif bit > 1:
            far = xor_swap(rest, "fs", bit)
            rest = jnp.concatenate([rest, near, far], axis=0)
            rels = rels + [bit] + [i ^ bit for i in rels]
        else:
            far = xor_swap(rest, "fs", bit)
            return [([bit], near), (rels, rest), ([i ^ bit for i in rels], far)]
        bit //= 2
    return [(rels, rest)]


def parity(r):
    return jnp.bitwise_xor(jnp.bitwise_and(r, 1), jnp.right_shift(r, 1))


def share(r):
    return (2 * parity(r), 2) if lax.axis_size("rep") == 4 else (r, 1)


def spread_planes(own):
    n_r = lax.axis_size("rep")
    pieces = []
    for m, part in enumerate(own):
        for n, (rels, got) in enumerate(spread(part)):
            pieces.append((rels, got, lambda r, m=m: share(r)[0] + m, n))
            if n_r != 4:
                for i in range(1, n_r):
                    near = xor_swap(got, "rep", i)
                    pieces.append((rels, near, lambda r, i=i: jnp.bitwise_xor(r, i), n))
            elif len(own) == 2 and m == 1 and len(rels) == 1 and n == 2 and got.shape[1] % 32 == 0:
                h = got.shape[1] // 2
                for i, half in enumerate((got[:, :h], got[:, h:])):
                    near = xor_swap(half, "rep", 1 + i)
                    pieces.append((rels, near, lambda r, i=i: (3 - 2 * parity(r), i), n))
            elif len(own) == 2:
                near = xor_swap(got, "rep", 1 + m)
                pieces.append((rels, near, lambda r, m=m: 2 + m - 2 * parity(r), n))
            else:
                h = got.shape[1] // 2
                for i, half in enumerate((got[:, :h], got[:, h:])):
                    near = xor_swap(half, "rep", 1 + i)
                    pieces.append((rels, near, lambda r, i=i: 2 + i - 2 * parity(r), n))
    return pieces


def spread_basis(basis_q, basis_k, r, t):
    n_f, n_r = lax.axis_size("fs"), lax.axis_size("rep")
    h = basis_q.shape[0] // n_r

    def rows(first, count):
        mine = (lax.dynamic_slice_in_dim(b, first * h, count * h, 0) for b in (basis_q, basis_k))
        return jnp.where(t == 0, *mine)

    first, count = share(r)
    if n_f != 4 or n_r != 4:
        return spread_planes([rows(first, count)])
    two = xor_swap(rows(r, 1)[None], "fs", 2)
    one = xor_swap(rows(first, count)[None], "fs", 1)
    three = xor_swap(two, "fs", 1)
    pieces = [([1], one, lambda r: share(r)[0], 0)]
    for i, half in enumerate((one[:, :h], one[:, h:])):
        near = xor_swap(half, "rep", 1 + i)
        pieces.append(([1], near, lambda r, i=i: 2 + i - 2 * parity(r), 0))
    for rel, got in ((2, two), (3, three)):
        pieces.append(([rel], got, lambda r: r, rel - 1))
        for i in range(1, n_r):
            near = xor_swap(got, "rep", i)
            pieces.append(([rel], near, lambda r, i=i: jnp.bitwise_xor(r, i), rel - 1))
    return pieces


def token_kernel(rels, z_ref, r_ref, t_ref, x_ref, own_q_ref, own_k_ref, *refs):
    parts, (basis_ref, token_ref) = refs[: len(rels)], refs[len(rels) : len(rels) + 2]
    x_vmem, x_sem, own_sem, sems = refs[len(rels) + 2 :]
    basis_vmem = basis_ref
    x_load = pltpu.make_async_copy(x_ref, x_vmem, x_sem)
    x_load.start()
    z = z_ref[0]
    rows = own_q_ref.shape[0]
    own_at = pl.ds(pl.multiple_of(z * rows, rows), rows)
    for query, source in ((True, own_q_ref), (False, own_k_ref)):

        @pl.when((t_ref[0] == 0) == query)
        def _():
            pltpu.make_async_copy(source, basis_vmem.at[own_at], own_sem).start()

    loads = []
    for n, ((rel, first), part) in enumerate(zip(rels, parts)):
        for j, rel_j in enumerate(rel):
            at = jnp.bitwise_xor(z, rel_j) * rows + first(r_ref[0]) * (rows // lax.axis_size("rep"))
            at = pl.ds(pl.multiple_of(at, 16), part.shape[1])
            loads.append(pltpu.make_async_copy(part.at[j], basis_vmem.at[at], sems.at[n, j]))
            loads[-1].start()
    x_load.wait()
    pltpu.make_async_copy(own_q_ref, basis_vmem.at[own_at], own_sem).wait()
    for load in loads:
        load.wait()
    token_ref[...] = jnp.dot(x_vmem[...], basis_vmem[...], preferred_element_type=F32).astype(BF)


def tokens(z, r, t, x, own_q, own_k, parts):
    shape = (x.shape[1], own_q.shape[1])
    hbm = pl.BlockSpec(memory_space=pltpu.HBM)
    token = (x.shape[0], own_q.shape[1])
    sources = (x, own_q, own_k, *[p for _, p, _, _ in parts])
    return pl.pallas_call(
        functools.partial(token_kernel, tuple((tuple(rel), first) for rel, _, first, _ in parts)),
        in_specs=[pl.BlockSpec(memory_space=pltpu.SMEM)] * 3 + [hbm] * len(sources),
        out_specs=[pl.BlockSpec(memory_space=pltpu.VMEM)] * 2,
        out_shape=[pltpu.VMEM(shape, BF), pltpu.VMEM(token, BF)],
        scratch_shapes=[
            pltpu.VMEM(x.shape, BF),
            pltpu.SemaphoreType.DMA,
            pltpu.SemaphoreType.DMA,
            pltpu.SemaphoreType.DMA((len(parts), max(len(rel) for rel, _, _, _ in parts))),
        ],
        compiler_params=SMALL,
        name="tokens",
    )(z, r, t, *[in_space(a, pltpu.HBM) for a in sources[:3]], *sources[3:])


def terms_kernel(t_ref, mine_ref, other_ref, cq_ref, ck_ref, out_ref):
    n_r, n_f, rows, _ = out_ref.shape
    cols_q = cq_ref.shape[1]
    query_mine = t_ref[0] == 0
    mine, other = mine_ref[...], other_ref[...]
    q = contract(jnp.where(query_mine, mine, other), cq_ref[...]).astype(BF)
    k = contract(jnp.where(query_mine, other, mine), ck_ref[...]).astype(BF)
    for j in range(n_f):
        for i in range(n_r):
            at = (j * n_r + i) * rows
            out_ref[i, j, :, :cols_q] = q[at : at + rows]
            out_ref[i, j, :, cols_q:] = k[at : at + rows]


def terms(t, mine, other, cot_q, cot_k):
    n_f, n_r = lax.axis_size("fs"), lax.axis_size("rep")
    shape = (n_r, n_f, mine.shape[1] // (n_f * n_r), cot_q.shape[1] + cot_k.shape[1])
    return pl.pallas_call(
        terms_kernel,
        in_specs=[pl.BlockSpec(memory_space=pltpu.SMEM)]
        + [whole(a) for a in (mine, other, cot_q, cot_k)],
        out_specs=whole(shape),
        grid=(1,),
        out_shape=pltpu.HBM(shape, BF),
        compiler_params=SMALL,
        name="terms",
    )(t, mine, other, cot_q, cot_k)


def sum_kernel(in_ref, out_ref):
    total = in_ref[0].astype(F32)
    for i in range(1, in_ref.shape[0]):
        total = total + in_ref[i].astype(F32)
    out_ref[...] = total.astype(BF)


def sum_first(value):
    return pl.pallas_call(
        sum_kernel,
        in_specs=[whole(value)],
        out_specs=whole(value.shape[1:]),
        grid=(1,),
        out_shape=pltpu.HBM(value.shape[1:], BF),
        compiler_params=SMALL,
        name="sum_first",
    )(value)


def moment_update(first, second, low):
    first = 0.9 * first + 0.1 * low
    second = 0.95 * second + 0.05 * low * low
    return first, second, first / (jnp.sqrt(second) + 1e-08)


def piece_kernel(got_ref, mq_ref, mk_ref, low_ref, out_ref):
    cols_q = mq_ref.shape[2]
    total = got_ref[0].astype(F32)
    for i in range(1, got_ref.shape[0]):
        total = total + got_ref[i].astype(F32)
    low = total.astype(BF)
    low_ref[...] = low
    low = low.astype(F32)
    q = moment_update(mq_ref[0], mq_ref[1], low[:, :cols_q])[2].astype(BF)
    k = moment_update(mk_ref[0], mk_ref[1], low[:, cols_q:])[2].astype(BF)
    for i in range(out_ref.shape[0]):
        out_ref[i, :, :cols_q] = q
        out_ref[i, :, cols_q:] = k


def piece(r, got, moments_q, moments_k):
    n_f, rows, cols = got.shape
    moments_q = lax.dynamic_slice_in_dim(moments_q, r * rows, rows, 1)
    moments_k = lax.dynamic_slice_in_dim(moments_k, r * rows, rows, 1)
    return pl.pallas_call(
        piece_kernel,
        in_specs=[whole(got), whole(moments_q), whole(moments_k)],
        out_specs=[whole((rows, cols)), whole((n_f, rows, cols))],
        grid=(1,),
        out_shape=[
            jax.ShapeDtypeStruct((rows, cols), BF),
            pltpu.HBM((n_f, rows, cols), BF),
        ],
        compiler_params=SMALL,
        name="piece",
    )(got, moments_q, moments_k)


def plane_kernel(z_ref, got_ref, low_ref, out_ref):
    for i in range(out_ref.shape[0]):
        out_ref[i] = got_ref[...]
        out_ref[i, z_ref[0]] = low_ref[...]


def plane(z, got, low):
    return pl.pallas_call(
        plane_kernel,
        in_specs=[pl.BlockSpec(memory_space=pltpu.SMEM), whole(got), whole(low)],
        out_specs=whole((lax.axis_size("rep"), *got.shape)),
        grid=(1,),
        out_shape=jax.ShapeDtypeStruct((lax.axis_size("rep"), *got.shape), BF),
        compiler_params=SMALL,
        name="plane",
    )(z, got, low)


def squares(value):
    rows, cols = value.shape
    total = jnp.sum(jnp.square(value).reshape(rows // 8, 8, cols), axis=0)
    parts = [total[:, i : i + 128] for i in range(0, cols, 128)]
    return functools.reduce(jnp.add, parts)


def directions_kernel(z_ref, got_ref, mq_ref, mk_ref, nq_ref, nk_ref, dq_ref, dk_ref, sums_ref):
    n_r, n_f, rows, _ = got_ref.shape
    cols_q = mq_ref.shape[2]
    z = z_ref[0]
    own = n_r * rows
    for j in range(n_f):
        got = jnp.concatenate([got_ref[i, j] for i in range(n_r)], axis=0)
        dq_ref[j * own : (j + 1) * own, :] = got[:, :cols_q]
        dk_ref[j * own : (j + 1) * own, :] = got[:, cols_q:]
    low = jnp.concatenate([got_ref[i, z] for i in range(n_r)], axis=0).astype(F32)
    q = moment_update(mq_ref[0], mq_ref[1], low[:, :cols_q])
    k = moment_update(mk_ref[0], mk_ref[1], low[:, cols_q:])
    nq_ref[0], nq_ref[1] = q[0], q[1]
    nk_ref[0], nk_ref[1] = k[0], k[1]
    at = pl.ds(pl.multiple_of(z * own, own), own)
    dq_ref[at, :] = q[2].astype(BF)
    dk_ref[at, :] = k[2].astype(BF)
    sums_ref[:8, :] = squares(dq_ref[...].astype(F32))
    sums_ref[8:, :] = squares(dk_ref[...].astype(F32))


def directions(z, got, moments_q, moments_k):
    n_r, n_f, rows, _ = got.shape
    rank = n_r * n_f * rows
    return pl.pallas_call(
        directions_kernel,
        in_specs=[pl.BlockSpec(memory_space=pltpu.SMEM), whole(got), whole(moments_q), whole(moments_k)],
        out_specs=[
            whole(moments_q),
            whole(moments_k),
            whole((rank, moments_q.shape[2])),
            whole((rank, moments_k.shape[2])),
            whole((16, 128)),
        ],
        grid=(1,),
        out_shape=[
            jax.ShapeDtypeStruct(moments_q.shape, F32),
            jax.ShapeDtypeStruct(moments_k.shape, F32),
            pltpu.VMEM((rank, moments_q.shape[2]), BF),
            pltpu.VMEM((rank, moments_k.shape[2]), BF),
            pltpu.VMEM((16, 128), F32),
        ],
        compiler_params=SMALL,
        name="directions",
    )(z, got, moments_q, moments_k)


def gather_pieces(plan, slots, rel, r, pieces, to, sems):
    loads = []
    h = to.shape[1] // lax.axis_size("rep")
    for i, (rels, first) in enumerate(plan):
        if rel in rels:
            j = rels.index(rel)
            at = first(r)
            at = at[0] * h + at[1] * (h // 2) if isinstance(at, tuple) else at * h
            at = pl.ds(pl.multiple_of(at, 16), pieces[i].shape[1])
            loads.append(
                pltpu.make_async_copy(pieces[i].at[j], to.at[slots[rel], at], sems.at[i, j])
            )
            loads[-1].start()
    return loads


def slots_of(plan):
    rels = []
    for got, _ in plan:
        rels += [rel for rel in got if rel not in rels]
    return {rel: i for i, rel in enumerate(rels)}


def plan_of(pieces):
    return tuple((tuple(rels), first) for rels, _, first, _ in pieces)


def semaphores(plan):
    return pltpu.SemaphoreType.DMA((len(plan), max(len(rels) for rels, _ in plan)))


CHUNK = 256


def finish_kernel(
    plan, n_tp, z_ref, r_ref, t_ref, sums_ref, other_sums_ref, dq_ref, dk_ref,
    mine_ref, other_ref, wq_ref, wk_ref, *refs,
):
    n = len(plan)
    pieces, outs, results, copies_out = refs[:n], refs[n : n + 6], refs[n + 6 : n + 10], refs[n + 10 : n + 12]
    bases, weights, (last, basis_sem, weight_sem, out_sem, copy_sem, sems) = (
        refs[n + 12 : n + 14], refs[n + 14 : n + 16], refs[n + 16 :]
    )
    z = z_ref[0]
    rows, cols_q = wq_ref.shape
    cols_k = wk_ref.shape[1]
    rank = dq_ref.shape[0]
    slots = slots_of(plan)
    order = [*slots]
    order = [0, *order]

    def block(rel):
        return pl.ds(pl.multiple_of(jnp.bitwise_xor(z, rel) * rows, rows), rows)

    loads = {}
    weight_loads = [
        pltpu.make_async_copy(source, to, weight_sem.at[i])
        for i, (source, to) in enumerate(zip((wq_ref, wk_ref), weights))
    ]
    for step, rel in enumerate(order):
        for query in (True, False):

            @pl.when((t_ref[0] == 0) == query)
            def _():
                for mat, source in enumerate((mine_ref, other_ref) if query else (other_ref, mine_ref)):
                    pltpu.make_async_copy(
                        source.at[block(rel)], bases[mat].at[step], basis_sem.at[mat, step]
                    ).start()

        if rel == 0:
            for load in weight_loads:
                load.start()
        else:
            loads[rel] = gather_pieces(plan, slots, rel, r_ref[0], pieces, last, sems)

    def scale(at, cols):
        total = jnp.sum(sums_ref[at, :] + other_sums_ref[at, :], keepdims=True)
        return lax.rsqrt(total / (rank * cols * n_tp) + 1e-06)

    scales = scale(slice(0, 8), cols_q), scale(slice(8, 16), cols_k)
    directions = dq_ref, dk_ref
    stores = []

    def store(source, to, sem):
        stores.append(pltpu.make_async_copy(source, to, sem))
        stores[-1].start()

    for step, rel in enumerate(order):
        for load in loads.get(rel, []):
            load.wait()
        for mat, part in ((0, slice(0, cols_q)), (1, slice(cols_q, cols_q + cols_k))):
            pltpu.make_async_copy(
                mine_ref.at[block(rel)], bases[mat].at[step], basis_sem.at[mat, step]
            ).wait()
            if rel == 0:
                weight_loads[mat].wait()
            for top in range(0, rows, CHUNK):
                at = slice(top, min(rows, top + CHUNK))
                product = jnp.dot(
                    bases[mat][step, at], directions[mat][...], preferred_element_type=F32
                )
                if rel == 0:
                    product = scales[mat] * product
                    results[mat][at] = product
                    new = weights[mat][at] - 0.02 * product
                    results[2 + mat][at] = new
                else:
                    old = last[slots[rel], at, part]
                    new = old.astype(F32) - (0.02 * scales[mat]) * product
                copies_out[mat][step, at] = new.astype(BF)
            if rel == 0:
                store(results[mat], outs[mat], out_sem.at[mat])
                store(results[2 + mat], outs[2 + mat], out_sem.at[2 + mat])
            store(copies_out[mat].at[step], outs[4 + mat].at[block(rel)], copy_sem.at[mat, step])
    for one in stores:
        one.wait()


def finish(z, r, t, sums, other_sums, dir_q, dir_k, mine, other, weight_q, weight_k, pieces):
    n_f, n_tp = lax.axis_size("fs"), lax.axis_size("tp")
    rows, cols_q = weight_q.shape
    cols_k = weight_k.shape[1]
    rank = mine.shape[1]
    plan = plan_of(pieces)
    hbm = pl.BlockSpec(memory_space=pltpu.HBM)
    smem = pl.BlockSpec(memory_space=pltpu.SMEM)
    vmem = pl.BlockSpec(memory_space=pltpu.VMEM)
    shapes = [
        ((rows, cols_q), F32),
        ((rows, cols_k), F32),
        ((rows, cols_q), F32),
        ((rows, cols_k), F32),
        ((rows * n_f, cols_q), BF),
        ((rows * n_f, cols_k), BF),
    ]
    inside = [in_space(a, pltpu.VMEM) for a in (sums, other_sums, dir_q, dir_k, mine)]
    outside = [
        in_space(a, pltpu.HBM) for a in (other, weight_q, weight_k, *[p[1] for p in pieces])
    ]
    return pl.pallas_call(
        functools.partial(finish_kernel, plan, n_tp),
        in_specs=[smem] * 3 + [vmem] * len(inside) + [hbm] * len(outside),
        out_specs=[hbm] * 6,
        out_shape=[pltpu.HBM(*s) for s in shapes],
        scratch_shapes=[
            *[pltpu.VMEM(*s) for s in shapes[:4]],
            pltpu.VMEM((n_f, rows, cols_q), BF),
            pltpu.VMEM((n_f, rows, cols_k), BF),
            *[pltpu.VMEM((n_f, rows, rank), BF)] * 2,
            pltpu.VMEM((rows, cols_q), F32),
            pltpu.VMEM((rows, cols_k), F32),
            pltpu.VMEM((len(slots_of(plan)), rows, cols_q + cols_k), BF),
            pltpu.SemaphoreType.DMA((2, n_f)),
            pltpu.SemaphoreType.DMA((2,)),
            pltpu.SemaphoreType.DMA((4,)),
            pltpu.SemaphoreType.DMA((2, n_f)),
            semaphores(plan),
        ],
        compiler_params=LARGE,
        name="finish",
    )(z, r, t, *inside, *outside)


def on_device(
    inputs,
    cot_query,
    cot_key,
    basis_query,
    basis_key,
    weight_query,
    weight_key,
    moments_query,
    moments_key,
):
    n_r = lax.axis_size("rep")
    z, r, t = lax.axis_index("fs"), lax.axis_index("rep"), lax.axis_index("tp")
    own_rows, _ = basis_query.shape
    h = own_rows // n_r
    at_z, at_r, at_t = (i.astype(jnp.int32)[None] for i in (z, r, t))
    first, count = share(r)

    parts = spread_basis(basis_query, basis_key, r, t)

    mine = [
        jnp.concatenate(
            [
                lax.dynamic_slice_in_dim(w, (first + i) * h, h, 0).astype(BF)
                for w in (weight_query, weight_key)
            ],
            axis=1,
        )
        for i in range(count)
    ]
    pieces = spread_planes(mine)

    basis, token = tokens(at_z, at_r, at_t, inputs, basis_query, basis_key, parts)
    other_token = xor_swap(token, "tp", 1)
    other_basis = xor_swap(basis, "tp", 1)
    low = exchange(terms(at_t, token, other_token, cot_query, cot_key), "rep")
    low = exchange(sum_first(low), "fs")
    low, rows = piece(r, low, moments_query, moments_key)
    rows = plane(at_z, exchange(rows, "fs"), low)
    rows = exchange(rows, "rep")
    new_q, new_k, dir_q, dir_k, sums = directions(at_z, rows, moments_query, moments_key)
    other_sums = xor_swap(sums, "tp", 1)
    outs = finish(
        at_z, at_r, at_t, sums, other_sums, dir_q, dir_k,
        basis, other_basis, weight_query, weight_key, pieces,
    )
    return (*outs, new_q, new_k)


def solution(mesh):
    in_specs = (
        P(("fs", "rep"), None),
        P(("fs", "rep"), "tp"),
        P(("fs", "rep"), "tp"),
        P("fs", None),
        P("fs", None),
        P("fs", "tp"),
        P("fs", "tp"),
        P(None, "fs", "tp"),
        P(None, "fs", "tp"),
    )
    out_specs = (
        P("fs", "tp"),
        P("fs", "tp"),
        P("fs", "tp"),
        P("fs", "tp"),
        P(None, "tp"),
        P(None, "tp"),
        P(None, "fs", "tp"),
        P(None, "fs", "tp"),
    )

    return jax.shard_map(
        on_device, mesh=mesh, in_specs=in_specs, out_specs=out_specs, check_vma=False
    )
```
